32 devices in a mesh: fs: 8 (over z, core), tp: 4 (over y, x).
Axes of the slice: x: 2, y: 2, z: 4, core: 2. Of those that a mesh axis runs over, the one named last changes fastest.
Arguments:
- gate_pre: bfloat16 [8192, 5632], P('fs', 'tp'), may hold values from -6 to 6
- up_pre: bfloat16 [8192, 5632], P('fs', 'tp'), may hold values from -6 to 6
- gate_taps: bfloat16 [3, 5632], replicated, may hold values from -3.5 to 3.5
- up_taps: bfloat16 [3, 5632], replicated, may hold values from -3.5 to 3.5
- down_proj: bfloat16 [5632, 2048], P('tp', 'fs'), may hold values from -0.078125 to 0.078125
- cotangent: bfloat16 [8192, 2048], P(('fs', 'tp')), may hold values from -6 to 6
Outputs:
- gate_grad: bfloat16 [8192, 5632], P('fs', 'tp')
- up_grad: bfloat16 [8192, 5632], P('fs', 'tp')
- down_grad: float32 [5632, 2048], P('tp', 'fs')
- row_norms: float32 [5632], P('tp')
- tap_grads: float32 [2, 3, 5632], replicated
The draws below stay inside these ranges and needn't reach their ends.
All inputs are finite; a program needn't handle non-finite values.
Results may differ from the reference program's by a relative error of at most 0.0042.
Values may be sent and summed in bfloat16 or wider, within the bound.
A program may use at most 128 MiB of HBM per device.

```python
import math
import jax
import jax.numpy as jnp
from jax import lax

D = 2048
FF = 5632
TAPS = 3
TOKENS = 8192
N_TP = 4


def with_spikes(array, own_key, source, target, parts, factor):
    owner, partner = [(jnp.arange(array.shape[position]) // (array.shape[position] // parts)).reshape([-1 if axis == position else 1 for axis in range(array.ndim)]) for position in (source, target)]
    chosen = jax.random.permutation(own_key, parts)[partner]
    strong = (owner == chosen) | (owner == (partner + parts // 2) % parts)
    return jnp.where(strong, factor * array, array)


def steps_of(key, dims, cuts, low, high):
    loudness = 1.0
    for position, parts in cuts:
        heights = jax.random.uniform(jax.random.fold_in(jax.random.fold_in(key, 6), position), (parts,), jnp.float32, low / len(cuts), high / len(cuts))
        loudness = loudness * jnp.repeat(jnp.exp(heights), dims[position] // parts).reshape((-1,) + (1,) * (len(dims) - 1 - position))
    return loudness


def centred(own_key, extent, width, bound, shards=(), dtype=jnp.bfloat16):
    drawn = jax.random.normal(own_key, extent, jnp.float32) * width
    if len(shards) > 0:
        drawn = steps_of(own_key, extent, shards, -0.22, 0.18) * drawn
    return jnp.clip(drawn, min=-bound, max=bound).astype(dtype)


def bell_draw_with(rng, extent, deviation, most, cuts, heavy, held_as=jnp.bfloat16):
    array = deviation * jax.random.normal(rng, extent, jnp.float32)
    if cuts:
        array = array * steps_of(rng, extent, cuts, -0.22, 0.18)
    return jnp.clip(with_spikes(array, jax.random.fold_in(rng, 3), *heavy), -most, most).astype(held_as)


def setup_inputs(seed: int = 0) -> dict:
    key_of = jax.random.split(jax.random.key(seed), 7)
    gate_pre = centred(key_of[0], (TOKENS, FF), 1.0, 6.0, ((0, 8), (1, 4)))
    up_pre = centred(key_of[1], (TOKENS, FF), 1.0, 6.0, ((0, 8), (1, 4)))
    gate_taps = centred(key_of[2], (TAPS, FF), TAPS ** -0.5, 3.5)
    up_taps = centred(key_of[3], (TAPS, FF), TAPS ** -0.5, 3.5)
    down_proj = centred(key_of[4], (FF, D), FF ** -0.5, 0.078125, ((0, 4), (1, 8)))
    cotangent = bell_draw_with(key_of[5], (TOKENS, D), 1.0, 6.0, ((0, 32),), (0, 1, 32, 2.75))
    return dict(gate_pre=gate_pre, up_pre=up_pre, gate_taps=gate_taps, up_taps=up_taps, down_proj=down_proj, cotangent=cotangent)


def block_grads(gate_block, up_block, gate_tap_block, up_tap_block, down_block, cotangent):
    count = gate_block.shape[0]
    reach = TAPS - 1
    gate_taps_f = gate_tap_block.astype(jnp.float32)
    up_taps_f = up_tap_block.astype(jnp.float32)
    gate_padded = jnp.pad(gate_block.astype(jnp.float32), ((reach, 0), (0, 0)))
    up_padded = jnp.pad(up_block.astype(jnp.float32), ((reach, 0), (0, 0)))
    gate_conv = gate_taps_f[0] * gate_padded[0:count]
    up_conv = up_taps_f[0] * up_padded[0:count]
    for offset in range(1, TAPS):
        gate_conv = gate_conv + gate_taps_f[offset] * gate_padded[offset:offset + count]
        up_conv = up_conv + up_taps_f[offset] * up_padded[offset:offset + count]
    gate_sigmoid = jax.nn.sigmoid(gate_conv)
    gate_act = gate_conv * gate_sigmoid
    hidden = (gate_act * up_conv).astype(jnp.bfloat16)
    hidden_grad = jnp.dot(cotangent, down_block.T, preferred_element_type=jnp.float32)
    gate_conv_grad = hidden_grad * up_conv * gate_sigmoid * (1.0 + gate_conv * (1.0 - gate_sigmoid))
    up_conv_grad = hidden_grad * gate_act
    gate_grad_pad = jnp.pad(gate_conv_grad, ((0, reach), (0, 0)))
    up_grad_pad = jnp.pad(up_conv_grad, ((0, reach), (0, 0)))
    gate_grad = gate_taps_f[0] * gate_grad_pad[reach:reach + count]
    up_grad = up_taps_f[0] * up_grad_pad[reach:reach + count]
    for offset in range(1, TAPS):
        lead = reach - offset
        gate_grad = gate_grad + gate_taps_f[offset] * gate_grad_pad[lead:lead + count]
        up_grad = up_grad + up_taps_f[offset] * up_grad_pad[lead:lead + count]
    grad_scale = 1.0 / math.sqrt(TOKENS)
    gate_tap_terms = jnp.stack([lax.optimization_barrier(jnp.sum(gate_conv_grad * gate_padded[offset:offset + count], axis=0)) for offset in range(TAPS)])
    up_tap_terms = jnp.stack([lax.optimization_barrier(jnp.sum(up_conv_grad * up_padded[offset:offset + count], axis=0)) for offset in range(TAPS)])
    tap_terms = jnp.stack([gate_tap_terms, up_tap_terms]) * grad_scale
    down_term = jnp.dot(hidden.T, cotangent, preferred_element_type=jnp.float32) * grad_scale
    norms = lax.optimization_barrier(jnp.sum(down_term * down_term, axis=1)) / down_term.shape[1]
    return (gate_grad.astype(jnp.bfloat16), up_grad.astype(jnp.bfloat16), down_term, norms, tap_terms)

def reference(gate_pre, up_pre, gate_taps, up_taps, down_proj, cotangent):
    channels = FF // N_TP
    gate_blocks = gate_pre.reshape(TOKENS, N_TP, channels).transpose(1, 0, 2)
    up_blocks = up_pre.reshape(TOKENS, N_TP, channels).transpose(1, 0, 2)
    gate_tap_blocks = gate_taps.reshape(TAPS, N_TP, channels).transpose(1, 0, 2)
    up_tap_blocks = up_taps.reshape(TAPS, N_TP, channels).transpose(1, 0, 2)
    down_blocks = down_proj.reshape(N_TP, channels, D)
    gate_grad, up_grad, down_grad, row_norms, tap_grads = lax.map(lambda items: block_grads(items[0], items[1], items[2], items[3], items[4], cotangent), (gate_blocks, up_blocks, gate_tap_blocks, up_tap_blocks, down_blocks))
    gate_grad = gate_grad.transpose(1, 0, 2).reshape(TOKENS, FF)
    up_grad = up_grad.transpose(1, 0, 2).reshape(TOKENS, FF)
    down_grad = down_grad.reshape(FF, D)
    row_norms = row_norms.reshape(FF)
    tap_grads = tap_grads.transpose(1, 2, 0, 3).reshape(2, TAPS, FF)
    return (gate_grad, up_grad, down_grad, row_norms, tap_grads)
```

```python
import functools
import math

import jax
import jax.numpy as jnp
from jax import lax
from jax.experimental import pallas as pl
from jax.experimental.pallas import tpu as pltpu
from jax.sharding import PartitionSpec as P

MESH = pl.DeviceIdType.MESH


def snake(position, width):
    row, column = position // width, position % width
    return row * width + column + (row % 2) * (width - 1 - 2 * column)


def conv_of(ref, halo_ref, taps_ref, start, count, columns):
    reach = taps_ref.shape[0] - 1
    here = ref[pl.ds(start, count), columns].astype(jnp.float32)
    earlier = pl.multiple_of(jnp.maximum(start - 16, 0), 16)
    tail = ref[pl.ds(earlier, 16), columns].astype(jnp.float32)[8:]
    tail = jnp.where(start == 0, halo_ref[:, columns], tail)
    rows = jnp.concatenate([tail, here], axis=0)
    out = None
    for offset in range(reach + 1):
        lag = reach - offset
        shifted = pltpu.roll(rows, lag, 0)[8:] if lag else here
        term = taps_ref[offset : offset + 1, columns] * shifted
        out = term if out is None else out + term
    return out


def gather_kernel(
    chips,
    tps,
    cot_ref,
    down_ref,
    gate_ref,
    up_ref,
    gate_halo,
    up_halo,
    gate_taps,
    up_taps,
    cot_out,
    down_out,
    hidden_out,
    *sems,
):
    (ring_send, ring_recv, line_send, line_recv, pair_send, pair_recv, local_sem) = sems
    f, q = lax.axis_index("fs"), lax.axis_index("tp")
    z, core = f // 2, f % 2
    width = math.isqrt(tps)
    spot = snake(q, width)
    half_ring = tps // 2
    ring_next = (snake((spot + 1) % tps, width), snake((spot + tps - 1) % tps, width))
    rows = cot_ref.shape[0]
    cols = down_ref.shape[1]
    partner = z * 2 + 1 - core
    behind, ahead = z > 0, z < chips - 1

    barrier = pltpu.get_barrier_semaphore()
    for device in ({"tp": ring_next[0]}, {"tp": ring_next[1]}, {"fs": partner}):
        pl.semaphore_signal(barrier, inc=1, device_id=device, device_id_type=MESH)

    @pl.when(behind)
    def _():
        pl.semaphore_signal(barrier, inc=1, device_id={"fs": f - 2}, device_id_type=MESH)

    @pl.when(ahead)
    def _():
        pl.semaphore_signal(barrier, inc=1, device_id={"fs": f + 2}, device_id_type=MESH)

    pl.semaphore_wait(barrier, 4 + (z + chips - 1) // chips - (z + 1) // chips)

    def cot_rows(owner_spot, way, part):
        owner = snake((owner_spot + 2 * tps) % tps, width)
        if part:
            return pl.ds(owner * rows + way * (rows // 2), rows // 2)
        return pl.ds(owner * rows, rows)

    def ring_copy(step, way):
        sign = 1 - 2 * way
        part = step == half_ring
        where = cot_rows(spot - sign * (step - 1), way, part)
        if step == 1:
            src = cot_ref.at[pl.ds(way * (rows // 2), rows // 2)] if part else cot_ref
        else:
            src = cot_out.at[where]
        return pltpu.make_async_remote_copy(
            src_ref=src,
            dst_ref=cot_out.at[where],
            send_sem=ring_send.at[way, step - 1],
            recv_sem=ring_recv.at[way, step - 1],
            device_id={"tp": ring_next[way]},
            device_id_type=MESH,
        )

    def ring_landing(step, way):
        sign = 1 - 2 * way
        where = cot_rows(spot - sign * step, way, step == half_ring)
        return pltpu.make_async_remote_copy(
            src_ref=cot_out.at[where],
            dst_ref=cot_out.at[where],
            send_sem=ring_send.at[way, step - 1],
            recv_sem=ring_recv.at[way, step - 1],
            device_id={"tp": ring_next[way]},
            device_id_type=MESH,
        )

    def down_block(chip, which):
        block = chip * 2 + which
        if cols % 128:
            return down_out.at[block]
        return down_out.at[:, pl.ds(pl.multiple_of(block * cols, cols), cols)]

    def line_copy(step, way):
        sign = 1 - 2 * way
        where = down_block(z - sign * (step - 1), core)
        return pltpu.make_async_remote_copy(
            src_ref=down_ref if step == 1 else where,
            dst_ref=where,
            send_sem=line_send.at[way, step - 1],
            recv_sem=line_recv.at[way, step - 1],
            device_id={"fs": f + 2 * sign},
            device_id_type=MESH,
        )

    def line_landing(step, way):
        sign = 1 - 2 * way
        where = down_block(z - sign * step, core)
        return pltpu.make_async_remote_copy(
            src_ref=where,
            dst_ref=where,
            send_sem=line_send.at[way, step - 1],
            recv_sem=line_recv.at[way, step - 1],
            device_id={"fs": f + 2 * sign},
            device_id_type=MESH,
        )

    def pair_copy(step, way, which):
        sign = 1 - 2 * way
        where = down_block(z - sign * step, which)
        slot = step + way * (chips - 1)
        return pltpu.make_async_remote_copy(
            src_ref=down_ref if step == 0 else where,
            dst_ref=where,
            send_sem=pair_send.at[slot],
            recv_sem=pair_recv.at[slot],
            device_id={"fs": partner},
            device_id_type=MESH,
        )

    def has_landing(step, way):
        return z >= step if way == 0 else z + step < chips

    def has_copy(step, way):
        going = ahead if way == 0 else behind
        return going if step == 1 else jnp.logical_and(going, has_landing(step - 1, way))

    for way in range(2):
        ring_copy(1, way).start()

        @pl.when(has_copy(1, way))
        def _():
            line_copy(1, way).start()

    pair_copy(0, 0, core).start()
    own_cot = pltpu.make_async_copy(cot_ref, cot_out.at[pl.ds(q * rows, rows)], local_sem.at[0])
    own_down = pltpu.make_async_copy(down_ref, down_block(z, core), local_sem.at[1])
    own_cot.start()
    own_down.start()

    total_rows, channels = gate_ref.shape
    count = math.gcd(total_rows, 64)

    def hidden_rows(i, carry):
        start = pl.multiple_of(i * count, count)
        for left in range(0, channels, 128):
            columns = pl.ds(left, min(128, channels - left))
            gate_conv = conv_of(gate_ref, gate_halo, gate_taps, start, count, columns)
            up_conv = conv_of(up_ref, up_halo, up_taps, start, count, columns)
            hidden = gate_conv * jax.nn.sigmoid(gate_conv) * up_conv
            hidden_out[pl.ds(start, count), columns] = hidden.astype(hidden_out.dtype)
        return carry

    lax.fori_loop(0, total_rows // count, hidden_rows, 0)

    for step in range(1, max(chips - 1, half_ring) + 1):
        if step <= chips - 1:
            for way in range(2):

                @pl.when(has_landing(step, way))
                def _():
                    line_landing(step, way).wait_recv()
                    pair_copy(step, way, core).start()

                if step + 1 <= chips - 1:

                    @pl.when(has_copy(step + 1, way))
                    def _():
                        line_copy(step + 1, way).start()

        if step <= half_ring:
            for way in range(2):
                ring_landing(step, way).wait_recv()
                if step + 1 <= half_ring:
                    ring_copy(step + 1, way).start()

    own_cot.wait()
    own_down.wait()
    pair_copy(0, 0, 1 - core).wait_recv()
    pair_copy(0, 0, core).wait_send()
    for way in range(2):
        for step in range(1, half_ring + 1):
            ring_copy(step, way).wait_send()
        for step in range(1, chips):

            @pl.when(has_copy(step, way))
            def _():
                line_copy(step, way).wait_send()

            @pl.when(has_landing(step, way))
            def _():
                pair_copy(step, way, 1 - core).wait_recv()
                pair_copy(step, way, core).wait_send()


def gather_both(cotangent, down_proj, *local):
    fs, tps = lax.axis_size("fs"), lax.axis_size("tp")
    chips = fs // 2
    rows, features = cotangent.shape
    channels, cols = down_proj.shape
    dma = pltpu.SemaphoreType.DMA
    down_shape = (fs, channels, cols) if cols % 128 else (channels, cols * fs)
    whole_cot, whole_down, hidden = pl.pallas_call(
        functools.partial(gather_kernel, chips, tps),
        out_shape=(
            jax.ShapeDtypeStruct((rows * tps, features), cotangent.dtype),
            jax.ShapeDtypeStruct(down_shape, down_proj.dtype),
            jax.ShapeDtypeStruct(local[0].shape, local[0].dtype),
        ),
        in_specs=[pl.BlockSpec(memory_space=pltpu.VMEM)] * (2 + len(local)),
        out_specs=[
            pl.BlockSpec(memory_space=pl.ANY),
            pl.BlockSpec(memory_space=pl.ANY),
            pl.BlockSpec(memory_space=pltpu.VMEM),
        ],
        scratch_shapes=[
            dma((2, tps // 2)),
            dma((2, tps // 2)),
            dma((2, chips - 1)),
            dma((2, chips - 1)),
            dma((2 * chips - 1,)),
            dma((2 * chips - 1,)),
            dma((2,)),
        ],
        compiler_params=pltpu.CompilerParams(collective_id=0, has_side_effects=True),
        name="gather_both",
    )(cotangent, down_proj, *local)
    if cols % 128:
        whole_down = whole_down.transpose(1, 0, 2).reshape(channels, fs * cols)
    return whole_cot, whole_down, hidden


def small_kernel(fs, tps, mine_ref, sum_ref, all_ref, terms, total, sums, *sems):
    send_a, recv_a, send_b, recv_b = sems
    f, q = lax.axis_index("fs"), lax.axis_index("tp")
    barrier = pltpu.get_barrier_semaphore()
    for i in range(1, fs):
        pl.semaphore_signal(
            barrier, inc=1, device_id={"fs": (f + i) % fs}, device_id_type=MESH
        )
    for i in range(1, tps):
        pl.semaphore_signal(
            barrier, inc=1, device_id={"tp": (q + i) % tps}, device_id_type=MESH
        )
    pl.semaphore_wait(barrier, fs + tps - 2)

    def over_fs(i):
        return pltpu.make_async_remote_copy(
            src_ref=mine_ref,
            dst_ref=terms.at[f],
            send_sem=send_a.at[i],
            recv_sem=recv_a.at[i],
            device_id={"fs": (f + i) % fs},
            device_id_type=MESH,
        )

    def over_tp(i):
        return pltpu.make_async_remote_copy(
            src_ref=total,
            dst_ref=sums.at[q],
            send_sem=send_b.at[i],
            recv_sem=recv_b.at[i],
            device_id={"tp": (q + i) % tps},
            device_id_type=MESH,
        )

    def landing(buffer, slot, send, recv, i, device):
        return pltpu.make_async_remote_copy(
            src_ref=buffer.at[slot],
            dst_ref=buffer.at[slot],
            send_sem=send.at[i],
            recv_sem=recv.at[i],
            device_id=device,
            device_id_type=MESH,
        )

    for i in range(1, fs):
        over_fs(i).start()
    terms[f] = mine_ref[...]
    for i in range(1, fs):
        landing(terms, (f + fs - i) % fs, send_a, recv_a, i, {"fs": (f + i) % fs}).wait_recv()
    added = terms[0]
    for i in range(1, fs):
        added = added + terms[i]
    total[...] = added
    sum_ref[...] = added
    sums[q] = added
    for i in range(1, fs):
        over_fs(i).wait_send()
    for i in range(1, tps):
        over_tp(i).start()
    for i in range(1, tps):
        landing(sums, (q + tps - i) % tps, send_b, recv_b, i, {"tp": (q + i) % tps}).wait_recv()
    all_ref[...] = sums[...]
    for i in range(1, tps):
        over_tp(i).wait_send()


def small_sums(mine, identity):
    fs, tps = lax.axis_size("fs"), lax.axis_size("tp")
    dma = pltpu.SemaphoreType.DMA
    shape = mine.shape
    return pl.pallas_call(
        functools.partial(small_kernel, fs, tps),
        out_shape=(
            jax.ShapeDtypeStruct(shape, jnp.float32),
            jax.ShapeDtypeStruct((tps,) + shape, jnp.float32),
        ),
        in_specs=[pl.BlockSpec(memory_space=pltpu.VMEM)],
        out_specs=[pl.BlockSpec(memory_space=pltpu.VMEM)] * 2,
        scratch_shapes=[
            pltpu.VMEM((fs,) + shape, jnp.float32),
            pltpu.VMEM(shape, jnp.float32),
            pltpu.VMEM((tps,) + shape, jnp.float32),
            dma((fs,)),
            dma((fs,)),
            dma((tps,)),
            dma((tps,)),
        ],
        compiler_params=pltpu.CompilerParams(collective_id=identity, has_side_effects=True),
        name=f"small_sums_{identity}",
    )(mine)


def norm_kernel(fs, mine_ref, sum_ref, terms, send, recv):
    f = lax.axis_index("fs")
    barrier = pltpu.get_barrier_semaphore()
    for i in range(1, fs):
        pl.semaphore_signal(
            barrier, inc=1, device_id={"fs": (f + i) % fs}, device_id_type=MESH
        )
    pl.semaphore_wait(barrier, fs - 1)

    def copy(i, src, slot):
        return pltpu.make_async_remote_copy(
            src_ref=src,
            dst_ref=terms.at[slot],
            send_sem=send.at[i],
            recv_sem=recv.at[i],
            device_id={"fs": (f + i) % fs},
            device_id_type=MESH,
        )

    for i in range(1, fs):
        copy(i, mine_ref, f).start()
    terms[f] = mine_ref[...]
    for i in range(1, fs):
        slot = (f + fs - i) % fs
        copy(i, terms.at[slot], slot).wait_recv()
    added = terms[0]
    for i in range(1, fs):
        added = added + terms[i]
    sum_ref[...] = added
    for i in range(1, fs):
        copy(i, mine_ref, f).wait_send()


def norm_sum(mine, identity):
    fs = lax.axis_size("fs")
    dma = pltpu.SemaphoreType.DMA
    return pl.pallas_call(
        functools.partial(norm_kernel, fs),
        out_shape=jax.ShapeDtypeStruct(mine.shape, jnp.float32),
        in_specs=[pl.BlockSpec(memory_space=pltpu.VMEM)],
        out_specs=pl.BlockSpec(memory_space=pltpu.VMEM),
        scratch_shapes=[pltpu.VMEM((fs,) + mine.shape, jnp.float32), dma((fs,)), dma((fs,))],
        compiler_params=pltpu.CompilerParams(collective_id=identity, has_side_effects=True),
        name="norm_sum",
    )(mine)


def from_behind(block, axis, distance):
    devices = range(lax.axis_size(axis))
    route = [(i - distance, i) for i in devices if i - distance in devices]
    return lax.ppermute(block, axis, route)


def body(gate_pre, up_pre, gate_taps, up_taps, down_proj, cotangent):
    row_count = gate_pre.shape[0]
    channels = gate_pre.shape[1]
    tap_count = gate_taps.shape[0]
    reach = tap_count - 1
    channel_start = lax.axis_index("tp") * channels
    gate_taps_f = lax.dynamic_slice_in_dim(gate_taps, channel_start, channels, 1).astype(
        jnp.float32
    )
    up_taps_f = lax.dynamic_slice_in_dim(up_taps, channel_start, channels, 1).astype(jnp.float32)
    before = from_behind((gate_pre[row_count - reach :], up_pre[row_count - reach :]), "fs", 1)
    halo = [
        jnp.concatenate([jnp.zeros((8 - reach, channels), jnp.float32), part.astype(jnp.float32)])
        for part in before
    ]
    whole_cot, whole_down, hidden = gather_both(
        cotangent, down_proj, gate_pre, up_pre, halo[0], halo[1], gate_taps_f, up_taps_f
    )
    grad_scale = 1.0 / math.sqrt(row_count * lax.axis_size("fs"))
    fs = lax.axis_size("fs")
    sum_type = jnp.bfloat16 if fs <= 8 else jnp.float32
    core = lax.axis_index("fs") % 2
    every_term = lax.dot_general(
        whole_cot, hidden, (((0,), (0,)), ((), ())), preferred_element_type=jnp.float32
    ).reshape(fs // 2, 2, -1, channels)

    def terms_of(which):
        return lax.dynamic_index_in_dim(every_term, which, 1, keepdims=False).reshape(-1, channels)

    given = terms_of(1 - core).astype(sum_type)
    taken = lax.ppermute(given, "fs", [(i, i ^ 1) for i in range(fs)])
    terms = (terms_of(core) + taken.astype(jnp.float32)).astype(sum_type)
    terms, whole_down, gate_pre, up_pre, before = lax.optimization_barrier(
        (terms, whole_down, gate_pre, up_pre, before)
    )
    groups = [list(range(which, fs, 2)) for which in range(2)]
    own_rows = lax.psum_scatter(
        terms, "fs", scatter_dimension=0, tiled=True, axis_index_groups=groups
    )
    own_rows = own_rows.astype(jnp.float32) * grad_scale
    gate_padded = jnp.concatenate([before[0], gate_pre], axis=0).astype(jnp.float32)
    up_padded = jnp.concatenate([before[1], up_pre], axis=0).astype(jnp.float32)
    gate_conv = gate_taps_f[0] * gate_padded[0:row_count]
    up_conv = up_taps_f[0] * up_padded[0:row_count]
    for offset in range(1, tap_count):
        gate_conv = gate_conv + gate_taps_f[offset] * gate_padded[offset : offset + row_count]
        up_conv = up_conv + up_taps_f[offset] * up_padded[offset : offset + row_count]
    gate_sigmoid = jax.nn.sigmoid(gate_conv)
    gate_act = gate_conv * gate_sigmoid
    hidden_grad = lax.dot_general(
        whole_cot,
        whole_down,
        (((1,), (1,)), ((), ())),
        preferred_element_type=jnp.float32,
    )
    gate_conv_grad = hidden_grad * up_conv * gate_sigmoid * (1.0 + gate_conv * (1.0 - gate_sigmoid))
    up_conv_grad = hidden_grad * gate_act
    following = from_behind((gate_conv_grad[0:reach], up_conv_grad[0:reach]), "fs", -1)
    gate_grad_pad = jnp.concatenate([gate_conv_grad, following[0]], axis=0)
    up_grad_pad = jnp.concatenate([up_conv_grad, following[1]], axis=0)
    gate_grad = gate_taps_f[0] * gate_grad_pad[reach : reach + row_count]
    up_grad = up_taps_f[0] * up_grad_pad[reach : reach + row_count]
    for offset in range(1, tap_count):
        lead = reach - offset
        gate_grad = gate_grad + gate_taps_f[offset] * gate_grad_pad[lead : lead + row_count]
        up_grad = up_grad + up_taps_f[offset] * up_grad_pad[lead : lead + row_count]
    gate_tap_terms = jnp.stack(
        [
            jnp.sum(gate_conv_grad * gate_padded[offset : offset + row_count], axis=0)
            for offset in range(tap_count)
        ]
    )
    up_tap_terms = jnp.stack(
        [
            jnp.sum(up_conv_grad * up_padded[offset : offset + row_count], axis=0)
            for offset in range(tap_count)
        ]
    )
    tap_terms = jnp.stack([gate_tap_terms, up_tap_terms])
    feature_count = whole_cot.shape[1]
    down_grad = own_rows.T
    partial_norms = jnp.sum(own_rows * own_rows, axis=0)
    tap_rows = tap_terms.reshape(2 * tap_count, channels)
    spare = jnp.zeros((-(2 * tap_count) % 8, channels), jnp.float32)
    _, everywhere = small_sums(jnp.concatenate([tap_rows, spare], axis=0), 1)
    row_norms = norm_sum(partial_norms[None], 2)[0] / feature_count
    tap_grads = (
        everywhere[:, : 2 * tap_count].transpose(1, 0, 2).reshape(2, tap_count, -1) * grad_scale
    )
    return (
        gate_grad.astype(jnp.bfloat16),
        up_grad.astype(jnp.bfloat16),
        down_grad,
        row_norms,
        tap_grads,
    )


def solution(mesh):
    placed = (P("fs", "tp"), P("fs", "tp"), P(), P(), P("tp", "fs"), P(("fs", "tp"), None))
    return jax.shard_map(
        body,
        mesh=mesh,
        in_specs=placed,
        out_specs=(P("fs", "tp"), P("fs", "tp"), P("tp", "fs"), P("tp"), P()),
        check_vma=False,
    )
```
